128 devices in a mesh: sp: 16 (over z, y), fs: 4 (over x), tp: 2 (over core).
Axes of the slice: x: 4, y: 4, z: 4, core: 2. Of those that a mesh axis runs over, the one named last changes fastest.
Arguments:
- tokens: bfloat16 [4, 4096, 2048], P('fs', 'sp', 'tp'), may hold values from -6 to 6
- norm_gain: float32 [2048], replicated, may hold values from 0.1 to 1.9
- lin_query: bfloat16 [2048, 1024], P(None, ('fs', 'tp')), may hold values from -0.125 to 0.125
- lin_key: bfloat16 [2048, 1024], P(None, ('fs', 'tp')), may hold values from -0.125 to 0.125
- lin_value: bfloat16 [2048, 2048], P(None, ('fs', 'tp')), may hold values from -0.125 to 0.125
- lin_decay: bfloat16 [2048, 1024], P(None, ('fs', 'tp')), may hold values from -0.125 to 0.125
- decay_bias: float32 [1024], replicated, may hold values from -0.5 to 8.5
- decay_shift: bfloat16 [2, 4, 4096], P(None, 'fs', 'sp'), may hold values from -1.4 to 1.5, as said below
- soft_query: bfloat16 [2048, 2048], P(None, ('fs', 'tp')), may hold values from -0.190034947 to 0.190034947
- soft_key: bfloat16 [2048, 2048], P(None, ('fs', 'tp')), may hold values from -1.9887378 to 1.9887378
- soft_value: bfloat16 [2048, 2048], P(None, ('fs', 'tp')), may hold values from -0.125 to 0.125
- soft_lambda: float32 [8], replicated, may hold values from 0.3 to 0.8
- lin_gain: float32 [256], replicated, may hold values from 0.1 to 1.9
- soft_gain: float32 [256], replicated, may hold values from 0.1 to 1.9
- lin_out: bfloat16 [2048, 2048], P(('fs', 'tp')), may hold values from -0.09375 to 0.09375
- soft_out: bfloat16 [2048, 2048], P(('fs', 'tp')), may hold values from -0.09375 to 0.09375
Outputs:
- mixed: bfloat16 [4, 4096, 2048], P('fs', 'sp', 'tp')
- log_mass: float32 [8, 2, 4, 4096], P(('fs', 'tp'), None, None, 'sp')
The draws below stay inside these ranges and needn't reach their ends.
Inputs may be any that keep to these rules, and one draw needn't show every extreme that they name: `decay_shift`: row 1 is never positive.
All inputs are finite; a program needn't handle non-finite values.
Results may differ from the reference program's by a relative error of at most 0.02.
Values may be sent and summed in bfloat16 or wider, within the bound.
No kernel may reach another device: no remote copies, remote signals or barrier semaphores. Data moves between devices by JAX's collectives and lax.ppermute only.
A program may use at most 192 MiB of HBM per device.

```python
import jax
import jax.numpy as jnp
from jax import lax

D = 2048
GLA_HEADS = 8
GLA_KEY = 128
GLA_VALUE = 256
DIFF_HEADS = 8
DIFF_HEAD = 128
DIFF_VALUE = 256
BLOCK = 64
TOK_DEV = 256
SEQUENCE_LENGTH = 4096
BATCH_SEQUENCES = 4


def draw_decay_bias(key, part):
    slow_share = 0.5
    slow_heads = jax.random.bernoulli(jax.random.fold_in(key, 201), slow_share, (GLA_HEADS,)).astype(jnp.float32)
    jitter = jax.random.uniform(jax.random.fold_in(key, 202), (GLA_HEADS, GLA_KEY), jnp.float32, -0.5, 0.5)
    return (8.0 * slow_heads[:, None] + jitter).reshape(GLA_HEADS * GLA_KEY)


def draw_decay_shift(key, part):
    level_count = SEQUENCE_LENGTH // TOK_DEV
    levels = jax.random.uniform(jax.random.fold_in(key, 301), (BATCH_SEQUENCES, level_count), jnp.float32, -0.8, 0.8)
    jitter = jax.random.uniform(jax.random.fold_in(key, 302), (BATCH_SEQUENCES, SEQUENCE_LENGTH), jnp.float32, -0.3, 0.3)
    gate_vector_row = jnp.repeat(levels, TOK_DEV, axis=1) + jitter
    spurt_position = jax.random.randint(jax.random.fold_in(key, 303), (BATCH_SEQUENCES, 3), 0, SEQUENCE_LENGTH)
    spurt_depth = jnp.log(jax.random.uniform(jax.random.fold_in(key, 304), (BATCH_SEQUENCES, 3), jnp.float32, 0.5, 0.8))
    match_count = jnp.arange(SEQUENCE_LENGTH, dtype=jnp.int32)[None, None, :] == spurt_position[:, :, None]
    spurt_row = jnp.sum(jnp.where(match_count, spurt_depth[:, :, None], 0.0), axis=1)
    return jnp.stack([gate_vector_row, spurt_row]).astype(jnp.bfloat16)


def query_table(key):
    raw_draw = jnp.clip(jax.random.normal(jax.random.fold_in(key, 101), (D, DIFF_HEADS * 2 * DIFF_HEAD), jnp.float32), -6.0, 6.0)
    return raw_draw * (2.0 / D) ** 0.5


def draw_soft_query(key, part):
    return query_table(key).astype(jnp.bfloat16)


def draw_soft_key(key, part):
    own_draw = jnp.clip(jax.random.normal(jax.random.fold_in(key, 102), (D, DIFF_HEADS * 2 * DIFF_HEAD), jnp.float32), -6.0, 6.0)
    own_draw = own_draw * (2.0 / D) ** 0.5
    result = own_draw
    return result.astype(jnp.bfloat16)


def block_scale(rng, extent, pieces, smallest, top_value):
    factor_of = 1.0
    for position, shards_of in pieces:
        steps = jax.random.uniform(jax.random.fold_in(jax.random.fold_in(rng, 6), position), (shards_of,), jnp.float32, smallest / len(pieces), top_value / len(pieces))
        factor_of = factor_of * jnp.repeat(jnp.exp(steps), extent[position] // shards_of).reshape((-1,) + (1,) * (len(extent) - 1 - position))
    return factor_of


def gaussian(stream_key, dims, scale, most, pieces=(), kind=jnp.bfloat16):
    drawn = scale * jax.random.normal(stream_key, dims, jnp.float32)
    if pieces:
        drawn = drawn * block_scale(stream_key, dims, pieces, -0.22, 0.18)
    return jnp.clip(drawn, -most, most).astype(kind)


def setup_inputs(seed: int = 0) -> dict:
    keys = jax.random.split(jax.random.key(seed), 17)
    tokens = gaussian(keys[0], (BATCH_SEQUENCES, SEQUENCE_LENGTH, D), 1.0, 6.0, ((0, 4), (1, 16), (2, 2)))
    norm_gain = jnp.clip(1.0 + 0.18 * jax.random.normal(keys[1], (D,), jnp.float32), 0.1, 1.9)
    lin_query = gaussian(keys[2], (D, GLA_HEADS * GLA_KEY), D ** -0.5, 0.125, ((1, 8),))
    lin_key = gaussian(keys[3], (D, GLA_HEADS * GLA_KEY), D ** -0.5, 0.125, ((1, 8),))
    lin_value = gaussian(keys[4], (D, GLA_HEADS * GLA_VALUE), D ** -0.5, 0.125, ((1, 8),))
    lin_decay = gaussian(keys[5], (D, GLA_HEADS * GLA_KEY), D ** -0.5, 0.125, ((1, 8),))
    decay_bias = draw_decay_bias(jax.random.fold_in(keys[16], 71), 0)
    decay_shift = draw_decay_shift(jax.random.fold_in(keys[16], 71), 0)
    soft_query = draw_soft_query(jax.random.fold_in(keys[16], 71), 0)
    soft_key = draw_soft_key(jax.random.fold_in(keys[16], 71), 0)
    soft_value = gaussian(keys[10], (D, DIFF_HEADS * DIFF_VALUE), D ** -0.5, 0.125, ((1, 8),))
    soft_lambda = jnp.clip(jax.random.uniform(keys[11], (DIFF_HEADS,), jnp.float32, 0.3, 0.8), 0.3, 0.8)
    lin_gain = jnp.clip(1.0 + 0.18 * jax.random.normal(keys[12], (GLA_VALUE,), jnp.float32), 0.1, 1.9)
    soft_gain = jnp.clip(1.0 + 0.18 * jax.random.normal(keys[13], (DIFF_VALUE,), jnp.float32), 0.1, 1.9)
    lin_out = gaussian(keys[14], (GLA_HEADS * GLA_VALUE, D), (GLA_HEADS * GLA_VALUE + DIFF_HEADS * DIFF_VALUE) ** -0.5, 0.09375, ((0, 8),))
    soft_out = gaussian(keys[15], (DIFF_HEADS * DIFF_VALUE, D), (GLA_HEADS * GLA_VALUE + DIFF_HEADS * DIFF_VALUE) ** -0.5, 0.09375, ((0, 8),))
    return dict(tokens=tokens, norm_gain=norm_gain, lin_query=lin_query, lin_key=lin_key, lin_value=lin_value, lin_decay=lin_decay, decay_bias=decay_bias, decay_shift=decay_shift, soft_query=soft_query, soft_key=soft_key, soft_value=soft_value, soft_lambda=soft_lambda, lin_gain=lin_gain, soft_gain=soft_gain, lin_out=lin_out, soft_out=soft_out)


norm_eps = 1e-06
decay_tau = 16.0
rope_base = 500000.0
highest = lax.Precision.HIGHEST

def scaled_rms(values, norm_gain):
    return values * lax.rsqrt(lax.optimization_barrier(jnp.mean(values * values, axis=-1, keepdims=True)) + norm_eps) * norm_gain

def rotate(values, positions):
    half_dim = values.shape[-1] // 2
    inv_freq = jnp.power(jnp.float32(rope_base), -jnp.arange(half_dim, dtype=jnp.float32) * (2.0 / values.shape[-1]))
    angles = positions.astype(jnp.float32)[:, None] * inv_freq[None, :]
    cos_table = jnp.cos(angles)[:, None, None, :]
    sin_table = jnp.sin(angles)[:, None, None, :]
    widened = values.astype(jnp.float32)
    first_half = widened[..., :half_dim]
    second_half = widened[..., half_dim:]
    turned = jnp.concatenate([first_half * cos_table - second_half * sin_table, second_half * cos_table + first_half * sin_table], axis=-1)
    return turned.astype(jnp.bfloat16)

def block_pass(queries, key_rows, value_rows, log_decay, block_len):
    groups, length, heads, key_dim = queries.shape
    value_dim = value_rows.shape[-1]
    block_count = length // block_len

    def split(tensor):
        return tensor.reshape(groups, block_count, block_len, heads, tensor.shape[-1]).transpose(1, 0, 3, 2, 4)
    causal = jnp.tril(jnp.ones((block_len, block_len), dtype=bool))[:, :, None]

    def advance(carry, inputs):
        state_now, offset = carry
        query_blk, key_blk, value_blk, decay_blk = inputs
        cum_log = jnp.cumsum(decay_blk, axis=2)
        inner_part = jnp.einsum('bhcd,bhdv->bhcv', query_blk * jnp.exp(cum_log), state_now, precision=highest)
        decay_pair = jnp.exp(jnp.where(causal, cum_log[:, :, :, None, :] - cum_log[:, :, None, :, :], -jnp.inf))
        scores = lax.optimization_barrier(jnp.sum(query_blk[:, :, :, None, :] * key_blk[:, :, None, :, :] * decay_pair, axis=-1))
        local_part = jnp.einsum('bhij,bhjv->bhiv', scores, value_blk, precision=highest)
        last_log = cum_log[:, :, -1, :]
        state_now = jnp.exp(last_log)[..., None] * state_now + jnp.einsum('bhcd,bhcv->bhdv', key_blk * jnp.exp(last_log[:, :, None, :] - cum_log), value_blk, precision=highest)
        carried = query_blk * jnp.exp(offset[:, :, None, :] + cum_log)
        return ((state_now, offset + last_log), (inner_part + local_part, carried))
    start = (jnp.zeros((groups, heads, key_dim, value_dim), jnp.float32), jnp.zeros((groups, heads, key_dim), jnp.float32))
    (state_end, offset_end), (outs, carried) = lax.scan(advance, start, (split(queries), split(key_rows), split(value_rows), split(log_decay)))
    return (outs, carried, state_end, offset_end)

def reference(tokens, norm_gain, lin_query, lin_key, lin_value, lin_decay, decay_bias, decay_shift, soft_query, soft_key, soft_value, soft_lambda, lin_gain, soft_gain, lin_out, soft_out):
    seq_count, seq_len, model_width = tokens.shape
    widened = tokens.astype(jnp.float32)
    normed = scaled_rms(widened, norm_gain).astype(jnp.bfloat16)
    flat_rows = normed.reshape(seq_count * seq_len, model_width)

    def project(weight):
        return jnp.dot(flat_rows, weight, preferred_element_type=jnp.float32)
    shift_rows = decay_shift.astype(jnp.float32)
    lin_q = project(lin_query).astype(jnp.bfloat16).reshape(seq_count, seq_len, GLA_HEADS, GLA_KEY)
    lin_k = project(lin_key).astype(jnp.bfloat16).reshape(seq_count, seq_len, GLA_HEADS, GLA_KEY)
    lin_v = project(lin_value).astype(jnp.bfloat16).reshape(seq_count, seq_len, GLA_HEADS, GLA_VALUE)
    gate_input = project(lin_decay) + decay_bias[None, :] + shift_rows[0].reshape(seq_count * seq_len)[:, None]
    log_decay = jax.nn.log_sigmoid(gate_input) / decay_tau + shift_rows[1].reshape(seq_count * seq_len)[:, None]
    log_decay = log_decay.reshape(seq_count, seq_len, GLA_HEADS, GLA_KEY)
    outs, carried, state_end, offset_end = block_pass(lin_q.astype(jnp.float32), lin_k.astype(jnp.float32), lin_v.astype(jnp.float32), log_decay, BLOCK)
    lin_raw = outs.transpose(1, 0, 3, 2, 4).reshape(seq_count, seq_len, GLA_HEADS, GLA_VALUE)
    lin_mix = scaled_rms(lin_raw, lin_gain).astype(jnp.bfloat16).reshape(seq_count * seq_len, GLA_HEADS * GLA_VALUE)
    positions = jnp.arange(seq_len, dtype=jnp.int32)
    soft_q = rotate(project(soft_query).astype(jnp.bfloat16).reshape(seq_count, seq_len, DIFF_HEADS, 2, DIFF_HEAD), positions)
    soft_k = rotate(project(soft_key).astype(jnp.bfloat16).reshape(seq_count, seq_len, DIFF_HEADS, 2, DIFF_HEAD), positions)
    soft_v = project(soft_value).astype(jnp.bfloat16).reshape(seq_count, seq_len, DIFF_HEADS, DIFF_VALUE)
    block_count = seq_len // TOK_DEV
    scale = DIFF_HEAD ** (-0.5)
    key_pos = jnp.arange(seq_len, dtype=jnp.int32)

    def attend(flat_index):
        seq_id = flat_index // block_count
        blk_id = flat_index % block_count
        seq_queries = lax.dynamic_index_in_dim(soft_q, seq_id, 0, keepdims=False)
        query_blk = lax.dynamic_slice_in_dim(seq_queries, blk_id * TOK_DEV, TOK_DEV, 0)
        seq_keys = lax.dynamic_index_in_dim(soft_k, seq_id, 0, keepdims=False)
        seq_values = lax.dynamic_index_in_dim(soft_v, seq_id, 0, keepdims=False)
        scores = jnp.einsum('qhmd,khmd->hmqk', query_blk.astype(jnp.float32), seq_keys.astype(jnp.float32)) * scale
        query_pos = blk_id * TOK_DEV + jnp.arange(TOK_DEV, dtype=jnp.int32)
        scores = jnp.where(key_pos[None, :] <= query_pos[:, None], scores, -jnp.inf)
        top = lax.optimization_barrier(jnp.max(scores, axis=-1, keepdims=True))
        expo = jnp.exp(scores - top)
        total = lax.optimization_barrier(jnp.sum(expo, axis=-1, keepdims=True))
        probs = expo / total
        mass = top[..., 0] + jnp.log(total[..., 0])
        weights = (probs[:, 0] - soft_lambda[:, None, None] * probs[:, 1]).astype(jnp.bfloat16)
        mixed_blk = jnp.einsum('hqk,khv->hqv', weights.astype(jnp.float32), seq_values.astype(jnp.float32))
        return (mixed_blk, mass)
    soft_raw, mass = lax.map(attend, jnp.arange(seq_count * block_count, dtype=jnp.int32))
    soft_raw = soft_raw.reshape(seq_count, block_count, DIFF_HEADS, TOK_DEV, DIFF_VALUE).transpose(0, 1, 3, 2, 4)
    soft_raw = soft_raw.reshape(seq_count, seq_len, DIFF_HEADS, DIFF_VALUE)
    soft_mix = scaled_rms(soft_raw, soft_gain).astype(jnp.bfloat16).reshape(seq_count * seq_len, DIFF_HEADS * DIFF_VALUE)
    log_mass = mass.reshape(seq_count, block_count, DIFF_HEADS, 2, TOK_DEV).transpose(2, 3, 0, 1, 4)
    log_mass = log_mass.reshape(DIFF_HEADS, 2, seq_count, seq_len)
    summed = jnp.dot(lin_mix, lin_out, preferred_element_type=jnp.float32) + jnp.dot(soft_mix, soft_out, preferred_element_type=jnp.float32)
    mixed = summed.astype(jnp.bfloat16).reshape(seq_count, seq_len, model_width)
    return (mixed, log_mass)
```

```python
import functools

import jax
import jax.numpy as jnp
from jax import lax
from jax.experimental import pallas as pl
from jax.experimental.pallas import tpu as pltpu
from jax.sharding import Mesh
from jax.sharding import PartitionSpec as P


KEY = 128
VALUE = 256
SP = ("sp_0", "sp_1")
GRID = ("sp_0", "sp_1", "tp")
ROW = ("fs", "tp")
ROWS = 256
EXTRA = 16

norm_eps = 1e-06
decay_tau = 16.0
rope_base = 500000.0
LOG2E = 1.4426950408889634
LN2 = 0.6931471805599453

NT = (((1,), (1,)), ((), ()))
TN = (((0,), (0,)), ((), ()))
bf16 = jnp.bfloat16
f32 = jnp.float32


def dot(a, b, dims=(((1,), (0,)), ((), ()))):
    return lax.dot_general(a, b, dims, preferred_element_type=f32)


def ring(length, shift):
    return [(i, (i + shift) % length) for i in range(length)]


def axis_perm(shift, first):
    pairs = []
    for z in range(4):
        for y in range(4):
            for c in range(2):
                along_z = (c == 0) == first
                tz, ty = ((z + shift) % 4, y) if along_z else (z, (y + shift) % 4)
                pairs.append(((z * 4 + y) * 2 + c, (tz * 4 + ty) * 2 + c))
    return pairs


def core_ring():
    return [(x * 2 + c, ((x + (1 if c == 0 else 3)) % 4) * 2 + c) for x in range(4) for c in range(2)]


def shift_fs(array, shift):
    return lax.ppermute(array, "fs", ring(4, shift))


def swap(array):
    return lax.ppermute(array, "tp", ring(2, 1))


def front_kernel(
    tok0, tok1, gain, w_lqk, w_lv, w_d, w_sq, w_sk, w_sv, bias, cos_t, sin_t,
    kv_out, q_out, local_out, carried_out, state_out,
):
    x0 = tok0[:ROWS, :].astype(f32)
    x1 = tok1[:ROWS, :].astype(f32)
    total = jnp.sum(x0 * x0, axis=1, keepdims=True) + jnp.sum(x1 * x1, axis=1, keepdims=True)
    inv = lax.rsqrt(total * (1.0 / 2048.0) + norm_eps)
    half = x0.shape[1]
    normed = jnp.concatenate(
        [(x0 * inv * gain[:, :half]).astype(bf16), (x1 * inv * gain[:, half:]).astype(bf16)], axis=1
    )
    cos_v = cos_t[...]
    sin_v = sin_t[...]

    def rotate(values):
        return values * cos_v + pltpu.roll(values, 64, 1) * sin_v

    sk = dot(normed, w_sk[...])
    for m in range(2):
        kv_out[:, m * KEY : (m + 1) * KEY] = rotate(sk[:, m * KEY : (m + 1) * KEY]).astype(bf16)
    kv_out[:, 2 * KEY :] = dot(normed, w_sv[...]).astype(bf16)
    sq = dot(normed, w_sq[...])
    scale = (KEY ** (-0.5)) * LOG2E
    for m in range(2):
        q_out[:, m * KEY : (m + 1) * KEY] = (rotate(sq[:, m * KEY : (m + 1) * KEY]) * scale).astype(bf16)

    shift0 = tok0[ROWS : ROWS + EXTRA, 0:ROWS]
    shift1 = tok0[ROWS : ROWS + EXTRA, ROWS : 2 * ROWS]
    pick = jnp.where(lax.broadcasted_iota(jnp.int32, (EXTRA, KEY), 0) == 0, 1.0, 0.0).astype(bf16)
    gate = dot(normed, w_d[...]) + bias[...] + dot(shift0, pick, TN)
    log_sig = jnp.minimum(gate, 0.0) - jnp.log1p(jnp.exp(-jnp.abs(gate)))
    log_decay = log_sig * (1.0 / decay_tau) + dot(shift1, pick, TN)

    lqk = dot(normed, w_lqk[...])
    q = lqk[:, :KEY].astype(bf16).astype(f32)
    k = lqk[:, KEY:].astype(bf16).astype(f32)
    v = dot(normed, w_lv[...]).astype(bf16)

    row = lax.broadcasted_iota(jnp.int32, (ROWS, KEY), 0)
    irow = lax.broadcasted_iota(jnp.int32, (ROWS, ROWS), 0)
    icol = lax.broadcasted_iota(jnp.int32, (ROWS, ROWS), 1)
    diff = irow ^ icol
    weights = jnp.where(irow == icol, jnp.sum(q * k, axis=1, keepdims=True), 0.0)
    inside = log_decay
    group = log_decay
    step = 1
    while step < ROWS:
        second = (row & step) != 0
        decay = jnp.exp(jnp.where(second, inside, group - inside))
        later = jnp.where(second, q * decay, 0.0).astype(bf16)
        earlier = jnp.where(second, 0.0, k * decay).astype(bf16)
        part = dot(later, earlier, NT)
        weights = weights + (part if 2 * step == ROWS else jnp.where(diff < 2 * step, part, 0.0))
        before = pltpu.roll(group, step, 0)
        after = pltpu.roll(group, ROWS - step, 0)
        inside = inside + jnp.where(second, before, 0.0)
        group = group + jnp.where(second, before, after)
        step *= 2
    local_out[...] = dot(weights.astype(bf16), v)
    carried_out[...] = (q * jnp.exp(inside)).astype(bf16)
    kept = (k * jnp.exp(group - inside)).astype(bf16)
    state_out[0:VALUE, :] = dot(v, kept, TN).astype(bf16)
    state_out[VALUE:, :] = jnp.exp(group[:EXTRA, :]).astype(bf16)


def front(tok0, tok1, *rest):
    shapes = (
        jax.ShapeDtypeStruct((ROWS, 4 * KEY), bf16),
        jax.ShapeDtypeStruct((ROWS, 2 * KEY), bf16),
        jax.ShapeDtypeStruct((ROWS, VALUE), f32),
        jax.ShapeDtypeStruct((ROWS, KEY), bf16),
        jax.ShapeDtypeStruct((VALUE + EXTRA, KEY), bf16),
    )
    return pl.pallas_call(
        front_kernel,
        out_shape=shapes,
        name="front",
        compiler_params=pltpu.CompilerParams(vmem_limit_bytes=40 * 1024 * 1024),
        cost_estimate=pl.CostEstimate(flops=1800000000, transcendentals=0, bytes_accessed=8000000),
    )(tok0, tok1, *rest)


def ordered(place, parts, j):
    k = (place - j) & 3
    value = parts[0]
    for n in range(1, 4):
        value = jnp.where(k == n, parts[n], value)
    return value


def prefix_kernel(place_ref, g0, g1, g2, g3, before_out, total_out):
    place = place_ref[0]
    parts = [g[0].astype(f32) for g in (g0, g1, g2, g3)]
    state = jnp.zeros((VALUE, KEY), f32)
    keep = jnp.ones((1, KEY), f32)
    before = state
    before_keep = keep
    for j in range(4):
        here = place == j
        before = jnp.where(here, state, before)
        before_keep = jnp.where(here, keep, before_keep)
        part = ordered(place, parts, j)
        own = part[VALUE : VALUE + 1, :]
        state = own * state + part[:VALUE, :]
        keep = own * keep
    before_out[0, :VALUE, :] = before
    before_out[0, VALUE:, :] = jnp.broadcast_to(before_keep, (EXTRA, KEY))
    total_out[0, :VALUE, :] = state.astype(bf16)
    total_out[0, VALUE:, :] = jnp.broadcast_to(keep, (EXTRA, KEY)).astype(bf16)


def prefix(place, parts):
    block = pl.BlockSpec((1, VALUE + EXTRA, KEY), lambda i, s: (i, 0, 0))
    shape = (4, VALUE + EXTRA, KEY)
    return pl.pallas_call(
        prefix_kernel,
        grid_spec=pltpu.PrefetchScalarGridSpec(
            num_scalar_prefetch=1, grid=(4,), in_specs=[block] * 4, out_specs=[block] * 2
        ),
        out_shape=(jax.ShapeDtypeStruct(shape, f32), jax.ShapeDtypeStruct(shape, bf16)),
        name="prefix",
    )(place, *parts)


def lin_kernel(place_ref, t0, t1, t2, t3, before, local, carried, gain, out):
    place = place_ref[0]
    parts = [t[0].astype(f32) for t in (t0, t1, t2, t3)]
    state = jnp.zeros((VALUE, KEY), f32)
    chosen = state
    for j in range(4):
        chosen = jnp.where(place == j, state, chosen)
        part = ordered(place, parts, j)
        state = part[VALUE : VALUE + 1, :] * state + part[:VALUE, :]
    state_in = before[0, VALUE : VALUE + 1, :] * chosen + before[0, :VALUE, :]
    raw = local[0] + dot(carried[0], state_in.astype(bf16), NT)
    mean = jnp.mean(raw * raw, axis=1, keepdims=True)
    out[0] = (raw * lax.rsqrt(mean + norm_eps) * gain[...]).astype(bf16)


def lin_final(place, totals, before, local, carried, gain):
    def block(rows, cols):
        return pl.BlockSpec((1, rows, cols), lambda i, s: (i, 0, 0))

    return pl.pallas_call(
        lin_kernel,
        grid_spec=pltpu.PrefetchScalarGridSpec(
            num_scalar_prefetch=1,
            grid=(4,),
            in_specs=[block(VALUE + EXTRA, KEY)] * 5
            + [block(ROWS, VALUE), block(ROWS, KEY), pl.BlockSpec((1, VALUE), lambda i, s: (0, 0))],
            out_specs=block(ROWS, VALUE),
        ),
        out_shape=jax.ShapeDtypeStruct((4, ROWS, VALUE), bf16),
        name="lin_final",
    )(place, *totals, before, local, carried, gain)


def attend_kernel(ids_ref, lam_ref, q_ref, own, low, high, far_a, far_b, gain, mix_out, mass_out, acc, top, total):
    g = pl.program_id(0)
    my_id = ids_ref[g]
    queries = [q_ref[0, :, m * KEY : (m + 1) * KEY] for m in range(2)]

    def scores(ref, index, m):
        return dot(queries[m], ref[index, :, m * KEY : (m + 1) * KEY], NT)

    irow = lax.broadcasted_iota(jnp.int32, (ROWS, ROWS), 0)
    icol = lax.broadcasted_iota(jnp.int32, (ROWS, ROWS), 1)
    values = own[g, :, 2 * KEY :]
    for m in range(2):
        s = jnp.where(icol <= irow, scores(own, g, m), -jnp.inf)
        peak = jnp.max(s, axis=1, keepdims=True)
        p = jnp.exp2(s - peak)
        top[m] = jnp.broadcast_to(peak, (ROWS, KEY))
        total[m] = jnp.broadcast_to(jnp.sum(p, axis=1, keepdims=True), (ROWS, KEY))
        acc[m] = dot(p.astype(bf16), values)

    def update(ref, index):
        vals = ref[index, :, 2 * KEY :]
        for m in range(2):
            s = scores(ref, index, m)
            old = top[m][:, 0:1]
            peak = jnp.maximum(old, jnp.max(s, axis=1, keepdims=True))
            p = jnp.exp2(s - peak)
            keep = jnp.exp2(old - peak)
            top[m] = jnp.broadcast_to(peak, (ROWS, KEY))
            total[m] = total[m] * keep + jnp.sum(p, axis=1, keepdims=True)
            acc[m] = acc[m] * keep + dot(p.astype(bf16), vals)

    def sweep(ref, first, start, stop, base):
        def body(j, carry):
            index = (j + first) & 3 if start else j

            @pl.when(ids_ref[base + index] < my_id)
            def _():
                update(ref, index)

            return carry

        lax.fori_loop(start, stop, body, 0)

    sweep(own, g, 1, 4, 0)
    sweep(low, 0, 0, 4, 4)
    sweep(high, 0, 0, 4, 8)
    sweep(far_a, 0, 0, 2, 12)
    sweep(far_b, 0, 0, 2, 14)

    raw = acc[0] * (1.0 / total[0][:, 0:1]) - acc[1] * (lam_ref[0] / total[1][:, 0:1])
    mean = jnp.mean(raw * raw, axis=1, keepdims=True)
    mix_out[0] = (raw * lax.rsqrt(mean + norm_eps) * gain[...]).astype(bf16)
    lane = lax.broadcasted_iota(jnp.int32, (ROWS, KEY), 1)
    mass = [LN2 * top[m] + jnp.log(total[m]) for m in range(2)]
    mass_out[0] = jnp.where(lane == 0, mass[0], mass[1]).T[:8, :]


def attend(ids, lam, queries, own, low, high, far_a, far_b, gain):
    def whole(n):
        return pl.BlockSpec((n, ROWS, 4 * KEY), lambda i, s, l: (0, 0, 0))

    return pl.pallas_call(
        attend_kernel,
        grid_spec=pltpu.PrefetchScalarGridSpec(
            num_scalar_prefetch=2,
            grid=(4,),
            in_specs=[
                pl.BlockSpec((1, ROWS, 2 * KEY), lambda i, s, l: (i, 0, 0)),
                whole(4), whole(4), whole(4), whole(2), whole(2),
                pl.BlockSpec((1, VALUE), lambda i, s, l: (0, 0)),
            ],
            out_specs=[
                pl.BlockSpec((1, ROWS, VALUE), lambda i, s, l: (i, 0, 0)),
                pl.BlockSpec((1, 8, ROWS), lambda i, s, l: (i, 0, 0)),
            ],
            scratch_shapes=[
                pltpu.VMEM((2, ROWS, VALUE), f32),
                pltpu.VMEM((2, ROWS, KEY), f32),
                pltpu.VMEM((2, ROWS, KEY), f32),
            ],
        ),
        out_shape=(
            jax.ShapeDtypeStruct((4, ROWS, VALUE), bf16),
            jax.ShapeDtypeStruct((4, 8, ROWS), f32),
        ),
        name="attend",
        compiler_params=pltpu.CompilerParams(vmem_limit_bytes=40 * 1024 * 1024),
    )(ids, lam, queries, own, low, high, far_a, far_b, gain)


def out_kernel(ids_ref, lin, soft, w_lin, w_soft, out):
    out[0] = (dot(lin[0], w_lin[...]) + dot(soft[0], w_soft[...])).astype(out.dtype)


def out_project(ids, lin_mix, soft_mix, lin_out, soft_out, count, kind):
    half = lin_out.shape[1] // 2

    def weight():
        return pl.BlockSpec((VALUE, half), lambda i, s: (0, s[2 * count]))

    return pl.pallas_call(
        out_kernel,
        grid_spec=pltpu.PrefetchScalarGridSpec(
            num_scalar_prefetch=1,
            grid=(count,),
            in_specs=[
                pl.BlockSpec((1, ROWS, VALUE), lambda i, s: (s[i], 0, 0)),
                pl.BlockSpec((1, ROWS, VALUE), lambda i, s: (s[count + i], 0, 0)),
                weight(), weight(),
            ],
            out_specs=pl.BlockSpec((1, ROWS, half), lambda i, s: (i, 0, 0)),
        ),
        out_shape=jax.ShapeDtypeStruct((count, ROWS, half), kind),
        name="out_project",
    )(ids, lin_mix, soft_mix, lin_out, soft_out)


def shards(
    tokens, norm_gain, lin_query, lin_key, lin_value, lin_decay, decay_bias, decay_shift,
    soft_query, soft_key, soft_value, soft_lambda, lin_gain, soft_gain, lin_out, soft_out,
):
    x = lax.axis_index("fs")
    c = lax.axis_index("tp")
    z = lax.axis_index("sp_0")
    y = lax.axis_index("sp_1")
    head = x * 2 + c
    width = tokens.shape[2]

    shift_row = decay_shift.reshape(1, 2 * ROWS)
    shift_row = jnp.pad(shift_row, ((0, EXTRA - 1), (0, width - 2 * ROWS)))
    own = jnp.concatenate([tokens[0], shift_row], axis=0)

    from_low = shift_fs(own, 1)
    from_high = shift_fs(own, 3)
    passed = jnp.where(c == 0, from_low, from_high)
    from_far = lax.ppermute(passed, ROW, core_ring())

    positions = (z * 4 + y) * ROWS + jnp.arange(ROWS, dtype=jnp.int32)
    inv_freq = jnp.power(f32(rope_base), -jnp.arange(64, dtype=f32) * (2.0 / KEY))
    angles = positions.astype(f32)[:, None] * inv_freq[None, :]
    cos = jnp.cos(angles)
    sin = jnp.sin(angles)
    cos_t = jnp.concatenate([cos, cos], axis=1)
    sin_t = jnp.concatenate([-sin, sin], axis=1)
    bias = lax.dynamic_slice_in_dim(decay_bias, head * KEY, KEY, 0).reshape(1, KEY)
    lam = lax.dynamic_slice_in_dim(soft_lambda, head, 1, 0)
    w_lqk = jnp.concatenate([lin_query, lin_key], axis=1)
    gain = norm_gain.reshape(1, -1)

    fronts = []
    for chunk in (own, from_high, from_far, from_low):
        other = swap(chunk)
        first = jnp.where(c == 0, chunk, other)
        second = jnp.where(c == 0, other, chunk)
        fronts.append(
            front(first, second, gain, w_lqk, lin_value, lin_decay, soft_query, soft_key, soft_value, bias, cos_t, sin_t)
        )
    kv, queries, local, carried, states = (jnp.stack(part) for part in zip(*fronts))

    r = jnp.where(c == 0, z, y)
    q = jnp.where(c == 0, y, z)

    def exchange(stacked):
        parts = []
        for k in range(4):
            piece = lax.dynamic_index_in_dim(stacked, (r + k - x) & 3, 0, keepdims=False)
            parts.append(piece if k == 0 else lax.ppermute(piece, GRID, axis_perm(k, True)))
        return jnp.stack(parts)

    own_kv = exchange(kv)
    my_q = exchange(queries)
    low_kv = lax.ppermute(own_kv, GRID, axis_perm(1, False))
    high_kv = lax.ppermute(own_kv, GRID, axis_perm(3, False))
    far_a = lax.ppermute(low_kv[:2], GRID, axis_perm(1, False))
    far_b = lax.ppermute(high_kv[2:], GRID, axis_perm(3, False))

    y_parts = [states] + [lax.ppermute(states, "sp_1", ring(4, k)) for k in (1, 2, 3)]
    before, totals = prefix(y.reshape(1), y_parts)
    z_parts = [totals] + [lax.ppermute(totals, "sp_0", ring(4, k)) for k in (1, 2, 3)]
    lin_mix = lin_final(z.reshape(1), z_parts, before, local, carried, lin_gain.reshape(1, -1))

    k4 = jnp.arange(4, dtype=jnp.int32)

    def block_ids(q_from, ks):
        p = (r - ks) & 3
        return jnp.where(c == 0, 4 * p + q_from, 4 * q_from + p)

    ids = jnp.concatenate(
        [
            block_ids(q, k4),
            block_ids((q - 1) & 3, k4),
            block_ids((q + 1) & 3, k4),
            block_ids((q + 2) & 3, k4),
        ]
    )
    mix, mass = attend(ids, lam, my_q, own_kv, low_kv, high_kv, far_a, far_b, soft_gain.reshape(1, -1))

    soft_mix = jnp.stack([mix[0]] + [lax.ppermute(mix[k], GRID, axis_perm(4 - k, True)) for k in (1, 2, 3)])
    mass_rows = jnp.stack(
        [mass[0, :2]] + [lax.ppermute(mass[k, :2], GRID, axis_perm(4 - k, True)) for k in (1, 2, 3)]
    )
    order = (jnp.arange(4, dtype=jnp.int32) - r) & 3
    log_mass = mass_rows[order].transpose(1, 0, 2)[None]

    def piece_ids(pieces, half):
        lin_ids = jnp.array(pieces, jnp.int32)
        return jnp.concatenate([lin_ids, (lin_ids + x - r) & 3, half.reshape(1)])

    def project(pieces, half, kind):
        return out_project(piece_ids(pieces, half), lin_mix, soft_mix, lin_out, soft_out, len(pieces), kind)

    far = project((2,), 1 - c, bf16)
    rest = project((1, 3, 0), 1 - c, bf16)
    far_in = swap(far)
    rest_in = swap(rest)
    mine = project((2, 1, 3, 0), c, f32)
    far_sum = (mine[0] + far_in[0].astype(f32)).astype(bf16)
    passed = lax.ppermute(far_sum, ROW, core_ring()).astype(f32)
    sums = mine[1:] + rest_in.astype(f32)
    up = (sums[0] + jnp.where(c == 0, passed, 0.0)).astype(bf16)
    down = (sums[1] + jnp.where(c == 0, 0.0, passed)).astype(bf16)
    mixed = sums[2] + shift_fs(up, 1).astype(f32) + shift_fs(down, 3).astype(f32)
    return (mixed.astype(bf16)[None], log_mass)


def solution(mesh):
    split = Mesh(
        mesh.devices.reshape(4, 4, mesh.shape["fs"], mesh.shape["tp"]), ("sp_0", "sp_1", "fs", "tp")
    )
    heads = P(None, ("fs", "tp"))
    placed = (
        P("fs", SP, "tp"), P(), heads, heads, heads, heads, P(), P(None, "fs", SP),
        heads, heads, heads, P(), P(), P(), P(("fs", "tp"), None), P(("fs", "tp"), None),
    )
    return jax.shard_map(
        shards,
        mesh=split,
        in_specs=placed,
        out_specs=(P("fs", SP, "tp"), P(("fs", "tp"), None, None, SP)),
        check_vma=False,
    )
```

```python
from functools import partial

import jax
import jax.numpy as jnp
from jax import lax
from jax.experimental import pallas as pl
from jax.experimental.pallas import tpu as pltpu
from jax.sharding import Mesh
from jax.sharding import PartitionSpec as P


KEY = 128
VALUE = 256
SP = ("sp_0", "sp_1")
GRID = ("sp_0", "sp_1", "tp")
ROW = ("fs", "tp")
ROWS = 256
EXTRA = 16

norm_eps = 1e-06
decay_tau = 16.0
rope_base = 500000.0
LOG2E = 1.4426950408889634
LN2 = 0.6931471805599453

NT = (((1,), (1,)), ((), ()))
TN = (((0,), (0,)), ((), ()))
bf16 = jnp.bfloat16
f32 = jnp.float32


def dot(a, b, dims=(((1,), (0,)), ((), ()))):
    return lax.dot_general(a, b, dims, preferred_element_type=f32)


def ring(length, shift):
    return [(i, (i + shift) % length) for i in range(length)]


def axis_perm(shift, first):
    pairs = []
    for z in range(4):
        for y in range(4):
            for c in range(2):
                along_z = (c == 0) == first
                tz, ty = ((z + shift) % 4, y) if along_z else (z, (y + shift) % 4)
                pairs.append(((z * 4 + y) * 2 + c, (tz * 4 + ty) * 2 + c))
    return pairs


def query_perm(k, back=False):
    pairs = []
    for p in range(4):
        for o in range(4):
            for c in range(2):
                tp, to = (p + k) % 4, o if p in (0, 3) else 3 - o
                here, there = ((p, o), (tp, to)) if c == 0 else ((o, p), (to, tp))
                pairs.append(tuple((i * 4 + j) * 2 + c for i, j in ((there, here) if back else (here, there))))
    return pairs


def core_ring(shift):
    return [(x * 2 + c, ((x + (shift if c == 0 else 4 - shift)) % 4) * 2 + c) for x in range(4) for c in range(2)]


def shift_fs(array, shift):
    return lax.ppermute(array, "fs", ring(4, shift))


def swap(array):
    return lax.ppermute(array, "tp", ring(2, 1))


def scalars():
    return pl.BlockSpec(memory_space=pltpu.SMEM)


def whole():
    return pl.BlockSpec(memory_space=pltpu.VMEM)


def params(mib):
    return pltpu.CompilerParams(vmem_limit_bytes=mib * 1024 * 1024)


def front_kernel(core_ref, mine, other, gain, w_sk, w_sv, w_sq, cos_t, sin_t, kv_out, q_out, normed_out):
    x0 = mine[...].astype(f32)
    x1 = other[...].astype(f32)
    total = jnp.sum(x0 * x0, axis=1, keepdims=True) + jnp.sum(x1 * x1, axis=1, keepdims=True)
    inv = lax.rsqrt(total * (1.0 / 2048.0) + norm_eps)
    half = x0.shape[1]
    here = pl.multiple_of(core_ref[0] * half, half)
    there = pl.multiple_of((1 - core_ref[0]) * half, half)
    normed_out[:, pl.ds(here, half)] = (x0 * inv * gain[:, pl.ds(here, half)]).astype(bf16)
    normed_out[:, pl.ds(there, half)] = (x1 * inv * gain[:, pl.ds(there, half)]).astype(bf16)
    normed = normed_out[...]
    cos_v = cos_t[...]
    sin_v = sin_t[...]

    def rotate(values):
        return values * cos_v + pltpu.roll(values, 64, 1) * sin_v

    sk = dot(normed, w_sk[...])
    for m in range(2):
        kv_out[:, m * KEY : (m + 1) * KEY] = rotate(sk[:, m * KEY : (m + 1) * KEY]).astype(bf16)
    kv_out[:, 2 * KEY :] = dot(normed, w_sv[...]).T.astype(bf16)
    sq = dot(normed, w_sq[...])
    scale = (KEY ** (-0.5)) * LOG2E
    for m in range(2):
        q_out[m * KEY : (m + 1) * KEY, :] = (rotate(sq[:, m * KEY : (m + 1) * KEY]) * scale).T.astype(bf16)


def front(*operands):
    return pl.pallas_call(
        front_kernel,
        in_specs=[scalars()] + [whole()] * (len(operands) - 1),
        out_shape=tuple(jax.ShapeDtypeStruct((ROWS, cols), bf16) for cols in (4 * KEY, 2 * KEY, 2048)),
        name="front",
        compiler_params=params(14),
        cost_estimate=pl.CostEstimate(flops=1500000000, transcendentals=0, bytes_accessed=6000000),
    )(*operands)


def gla_kernel(
    n0, n1, n2, n3, shifts, w_lv, w_d, w_lq, w_lk, bias, local_out, carried_out, state_out, normed_ref, w_lqk
):
    for n, source in enumerate((n0, n1, n2, n3)):
        normed_ref[n] = source[...]
    w_lqk[:, :KEY] = w_lq[...]
    w_lqk[:, KEY:] = w_lk[...]

    def one(n, carry):
        gla_chunk(
            normed_ref[n], shifts[n], w_lv, w_d, w_lqk, bias, local_out.at[n], carried_out.at[n], state_out.at[n]
        )
        return carry

    lax.fori_loop(0, 4, one, 0)


def gla_chunk(normed, shift, w_lv, w_d, w_lqk, bias, local_out, carried_out, state_out):
    pick = lax.broadcasted_iota(jnp.int32, (EXTRA, KEY), 0)
    pick0 = jnp.where(pick == 0, 1.0, 0.0).astype(bf16)
    pick1 = jnp.where(pick == 1, 1.0, 0.0).astype(bf16)
    gate = dot(normed, w_d[...]) + bias[...] + dot(shift, pick0, TN)
    log_sig = jnp.minimum(gate, 0.0) - jnp.log1p(jnp.exp(-jnp.abs(gate)))
    log_decay = log_sig * (1.0 / decay_tau) + dot(shift, pick1, TN)
    v = dot(normed, w_lv[...]).astype(bf16)
    lqk = dot(normed, w_lqk[...])
    q = lqk[:, :KEY].astype(bf16).astype(f32)
    k = lqk[:, KEY:].astype(bf16).astype(f32)

    row = lax.broadcasted_iota(jnp.int32, (ROWS, KEY), 0)
    irow = lax.broadcasted_iota(jnp.int32, (KEY, KEY), 0)
    icol = lax.broadcasted_iota(jnp.int32, (KEY, KEY), 1)
    diff = irow ^ icol
    itself = jnp.sum(q * k, axis=1, keepdims=True)
    halves = [jnp.where(diff == 0, itself[n * KEY : (n + 1) * KEY], 0.0) for n in range(2)]
    inside = log_decay
    group = log_decay
    step = 1
    while step < ROWS:
        second = (row & step) != 0
        decay = jnp.exp(jnp.where(second, inside, group - inside))
        scaled = (jnp.where(second, q, k) * decay).astype(bf16)
        if 2 * step == ROWS:
            cross = dot(scaled[KEY:], scaled[:KEY], NT)
        else:
            keep = (diff < 2 * step) & ((irow & step) != 0) & ((icol & step) == 0)
            for n in range(2):
                part = scaled[n * KEY : (n + 1) * KEY]
                halves[n] = halves[n] + jnp.where(keep, dot(part, part, NT), 0.0)
        before = pltpu.roll(group, step, 0)
        after = pltpu.roll(group, ROWS - step, 0)
        inside = inside + jnp.where(second, before, 0.0)
        group = group + jnp.where(second, before, after)
        step *= 2
    local_out[:KEY] = dot(halves[0].astype(bf16), v[:KEY])
    local_out[KEY:] = dot(jnp.concatenate([cross, halves[1]], axis=1).astype(bf16), v)
    carried_out[...] = (q * jnp.exp(inside)).astype(bf16)
    kept = (k * jnp.exp(group - inside)).astype(bf16)
    state_out[:VALUE, :] = dot(v, kept, TN).astype(bf16)
    state_out[VALUE:, :] = jnp.exp(group[:EXTRA, :]).astype(bf16)


def gla(normed, shifts, weights, bias):
    return pl.pallas_call(
        gla_kernel,
        in_specs=[whole()] * 10,
        out_shape=(
            jax.ShapeDtypeStruct((4, ROWS, VALUE), f32),
            jax.ShapeDtypeStruct((4, ROWS, KEY), bf16),
            jax.ShapeDtypeStruct((4, VALUE + EXTRA, KEY), bf16),
        ),
        scratch_shapes=[pltpu.VMEM((4, ROWS, 2048), bf16), pltpu.VMEM((2048, 2 * KEY), bf16)],
        name="gla",
        compiler_params=params(16),
        cost_estimate=pl.CostEstimate(flops=6000000000, transcendentals=0, bytes_accessed=9000000),
    )(*normed, shifts, *weights, bias)


def ordered(place, parts, j):
    k = (place - j) & 3
    value = parts[0]
    for n in range(1, 4):
        value = jnp.where(k == n, parts[n], value)
    return value


def prefix_kernel(place_ref, g0, g1, g2, g3, before_out, total_out):
    place = place_ref[0]
    parts = [g[...].astype(f32) for g in (g0, g1, g2, g3)]
    state = jnp.zeros((VALUE, KEY), f32)
    keep = jnp.ones((1, KEY), f32)
    for j in range(4):
        before_out[j, :VALUE, :] = state
        before_out[j, VALUE:, :] = jnp.broadcast_to(keep, (EXTRA, KEY))
        part = ordered(place, parts, j)
        own = part[VALUE : VALUE + 1, :]
        state = own * state + part[:VALUE, :]
        keep = own * keep
    total_out[:VALUE, :] = state.astype(bf16)
    total_out[VALUE:, :] = jnp.broadcast_to(keep, (EXTRA, KEY)).astype(bf16)


def prefix(place, parts):
    shape = (VALUE + EXTRA, KEY)
    return pl.pallas_call(
        prefix_kernel,
        in_specs=[scalars()] + [whole()] * 4,
        out_shape=(jax.ShapeDtypeStruct((4,) + shape, f32), jax.ShapeDtypeStruct(shape, bf16)),
        name="prefix",
        compiler_params=params(8),
    )(place, *parts)


def combine_kernel(place_ref, t0, t1, t2, t3, before, o0, o1, o2, o3):
    parts = [t[...].astype(f32) for t in (t0, t1, t2, t3)]
    state = jnp.zeros((VALUE, KEY), f32)
    chosen = state
    for j in range(4):
        chosen = jnp.where(place_ref[0] == j, state, chosen)
        part = ordered(place_ref[0], parts, j)
        state = part[VALUE : VALUE + 1, :] * state + part[:VALUE, :]
    for k, out in enumerate((o0, o1, o2, o3)):
        j = (place_ref[1] + k) & 3
        out[...] = (before[j, VALUE : VALUE + 1, :] * chosen + before[j, :VALUE, :]).astype(bf16)


def combine(places, totals, before):
    return pl.pallas_call(
        combine_kernel,
        in_specs=[scalars()] + [whole()] * 5,
        out_shape=tuple(jax.ShapeDtypeStruct((VALUE, KEY), bf16) for _ in range(4)),
        name="combine",
        compiler_params=params(8),
    )(places, *totals, before)


def lin_kernel(index_ref, i0, i1, i2, i3, local, carried, gain, out):
    for n in range(4):
        which = index_ref[n]
        state_in = i0[...]
        for m, later in enumerate((i1, i2, i3)):
            state_in = jnp.where(which == m + 1, later[...], state_in)
        raw = local[n] + dot(carried[n], state_in, NT)
        mean = jnp.mean(raw * raw, axis=1, keepdims=True)
        out[n] = (raw * lax.rsqrt(mean + norm_eps) * gain[...]).astype(bf16)


def lin_final(index, states, local, carried, gain):
    return pl.pallas_call(
        lin_kernel,
        in_specs=[scalars()] + [whole()] * 7,
        out_shape=jax.ShapeDtypeStruct((4, ROWS, VALUE), bf16),
        name="lin_final",
        compiler_params=params(12),
    )(index, *states, local, carried, gain)


def attend_kernel(near, ids_ref, slot_ids_ref, lam_ref, *refs):
    count_parts = 6 if near else 2
    q_refs, refs = refs[:4], refs[4:]
    parts, refs = refs[:count_parts], refs[count_parts:]
    if near:
        acc, top, total, items, q_all, kv, s_even, s_odd, p_even, p_odd, keep_even, keep_odd, sems = refs
    else:
        acc_in, top, total, gain, out0, out1, out2, out3, items, q_all, kv, s_even, s_odd, p_even, p_odd = refs[:15]
        keep_even, keep_odd, sems, acc, top_in, total_in, mass_ref, mix = refs[15:]
        top_in[...] = top[...]
        total_in[...] = total[...]
        top, total = top_in, total_in
        acc[...] = acc_in[...]
    copies = [
        pltpu.make_async_copy(source, kv.at[pl.ds(2 * n, 2)], sems.at[n]) for n, source in enumerate(parts)
    ]
    for copy in copies:
        copy.start()
    if near:
        acc[...] = jnp.zeros(acc.shape, f32)
        top[...] = jnp.full(top.shape, -jnp.inf, f32)
        total[...] = jnp.zeros(total.shape, f32)
    for n, source in enumerate(q_refs):
        q_all[n] = source[...]
    p_odd[...] = jnp.zeros(p_odd.shape, bf16)
    keep_odd[...] = jnp.ones(keep_odd.shape, f32)

    def collect(n, count):
        items[count] = n
        return count + jnp.where(slot_ids_ref[n >> 2] <= ids_ref[n & 3], 1, 0)

    count = lax.fori_loop(0, 8 * count_parts, collect, 0)
    visible = lax.broadcasted_iota(jnp.int32, (ROWS, ROWS), 0) <= lax.broadcasted_iota(jnp.int32, (ROWS, ROWS), 1)

    def item(i):
        n = items[i]
        return n >> 2, n & 3

    def arrive(slot, before):
        @pl.when((slot >> 1) != (before >> 1))
        def _():
            def wait(n, carry):
                pltpu.make_async_copy(parts[0], kv.at[pl.ds(2 * n, 2)], sems.at[n]).wait()
                return carry

            lax.fori_loop((before >> 1) + 1, (slot >> 1) + 1, wait, 0)

    def scores(after, slot, g, m):
        after[m] = dot(kv[slot, :, m * KEY : (m + 1) * KEY], q_all[g, m * KEY : (m + 1) * KEY, :])

    def mask(after, slot, g):
        @pl.when(slot_ids_ref[slot] == ids_ref[g])
        def _():
            for m in range(2):
                after[m] = jnp.where(visible, after[m], -jnp.inf)

    def weigh(now, p_now, keep_now, g, m):
        old = top[g, m][:1]
        peak = jnp.maximum(old, jnp.max(now[m], axis=0, keepdims=True))
        keep = jnp.exp2(old - peak)
        p = jnp.exp2(now[m] - peak)
        top[g, m] = jnp.broadcast_to(peak, (8, ROWS))
        total[g, m] = total[g, m] * keep + jnp.sum(p, axis=0, keepdims=True)
        keep_now[m] = jnp.broadcast_to(keep, (8, ROWS))
        p_now[m] = p.astype(bf16)

    def add(p_then, keep_then, slot, g, m):
        acc[g, m] = acc[g, m] * keep_then[m][:1] + dot(kv[slot, :, 2 * KEY :], p_then[m])

    def stage(i, now, after, p_now, p_then, keep_now, keep_then):
        slot_then, g_then = item(jnp.maximum(i - 1, 0))
        slot_now, g_now = item(i)
        slot_next, g_next = item(jnp.minimum(i + 1, count - 1))
        arrive(slot_next, slot_now)
        for m in range(2):
            scores(after, slot_next, g_next, m)
            weigh(now, p_now, keep_now, g_now, m)
            add(p_then, keep_then, slot_then, g_then, m)
        mask(after, slot_next, g_next)

    def run():
        first_slot, first_g = item(0)
        arrive(first_slot, -1)
        for m in range(2):
            scores(s_even, first_slot, first_g, m)
        mask(s_even, first_slot, first_g)

        def pair(n, carry):
            stage(2 * n, s_even, s_odd, p_even, p_odd, keep_even, keep_odd)

            @pl.when(2 * n + 1 < count)
            def _():
                stage(2 * n + 1, s_odd, s_even, p_odd, p_even, keep_odd, keep_even)

            return carry

        lax.fori_loop(0, (count + 1) >> 1, pair, 0)
        last_slot, last_g = item(count - 1)
        arrive(2 * count_parts - 1, last_slot)

        @pl.when((count & 1) == 1)
        def _():
            for m in range(2):
                add(p_even, keep_even, last_slot, last_g, m)

        @pl.when((count & 1) == 0)
        def _():
            for m in range(2):
                add(p_odd, keep_odd, last_slot, last_g, m)

    if near:
        pl.when(count > 0)(run)
        pl.when(count == 0)(lambda: arrive(2 * count_parts - 1, -1))
        return
    pl.when(count > 0)(run)
    pl.when(count == 0)(lambda: arrive(2 * count_parts - 1, -1))

    def finish(g, carry):
        sums = [total[g, m][:1] for m in range(2)]
        raw = acc[g, 0] * (1.0 / sums[0]) - acc[g, 1] * (lam_ref[0] / sums[1])
        mean = jnp.mean(raw * raw, axis=0, keepdims=True)
        mix[g, :ROWS] = ((raw * lax.rsqrt(mean + norm_eps)).T * gain[...]).astype(bf16)
        for m in range(2):
            left = jnp.broadcast_to(LN2 * top[g, m][:1] + jnp.log(sums[m]), (8, ROWS))
            lines = jnp.zeros((8, ROWS), f32)
            row = lax.broadcasted_iota(jnp.int32, (8, ROWS), 0)
            for n in range(3):
                part = left.astype(bf16).astype(f32)
                lines = jnp.where(row == n, part, lines)
                left = left - part
            mass_ref[m * 8 : (m + 1) * 8] = lines
        mix[g, ROWS:] = mass_ref[...].astype(bf16)
        return carry

    lax.fori_loop(0, 4, finish, 0)
    for n, out in enumerate((out0, out1, out2, out3)):
        out[...] = mix[n]


SUMS = ((4, 2, VALUE, ROWS), (4, 2, 8, ROWS), (4, 2, 8, ROWS))


def attend(near, ids, slot_ids, lam, queries, parts, *rest):
    scratch = [
        pltpu.SMEM((72,), jnp.int32),
        pltpu.VMEM((4, 2 * KEY, ROWS), bf16),
        pltpu.VMEM((2 * len(parts), ROWS, 4 * KEY), bf16),
        pltpu.VMEM((2, ROWS, ROWS), f32),
        pltpu.VMEM((2, ROWS, ROWS), f32),
        pltpu.VMEM((2, ROWS, ROWS), bf16),
        pltpu.VMEM((2, ROWS, ROWS), bf16),
        pltpu.VMEM((2, 8, ROWS), f32),
        pltpu.VMEM((2, 8, ROWS), f32),
        pltpu.SemaphoreType.DMA((len(parts),)),
    ]
    if near:
        out_shape = tuple(jax.ShapeDtypeStruct(shape, f32) for shape in SUMS)
    else:
        out_shape = tuple(jax.ShapeDtypeStruct((ROWS + EXTRA, VALUE), bf16) for _ in range(4))
        scratch += [pltpu.VMEM(shape, f32) for shape in SUMS]
        scratch += [pltpu.VMEM((EXTRA, ROWS), f32), pltpu.VMEM((4, ROWS + EXTRA, VALUE), bf16)]
    anywhere = pl.BlockSpec(memory_space=pl.ANY)
    return pl.pallas_call(
        partial(attend_kernel, near),
        in_specs=[scalars()] * 3 + [whole()] * 4 + [anywhere] * len(parts) + [whole()] * len(rest),
        out_shape=out_shape,
        scratch_shapes=scratch,
        name="attend_near" if near else "attend_far",
        compiler_params=params(18),
        cost_estimate=pl.CostEstimate(flops=4000000000, transcendentals=0, bytes_accessed=4000000),
    )(ids, slot_ids, lam, *queries, *parts, *rest)


def mixed_rows(index_ref, at, lin, lin_other, soft, soft_other):
    a = index_ref[at]
    b = index_ref[4 + at]
    e = index_ref[8 + at]
    return jnp.concatenate([lin[a], lin_other[a], soft[b, :ROWS], soft_other[e, :ROWS]], axis=1)


def send_kernel(index_ref, lin, lin_other, soft, soft_other, weight, far_out):
    far_out[...] = dot(mixed_rows(index_ref, 0, lin, lin_other, soft, soft_other), weight[...]).astype(bf16)


def keep_kernel(index_ref, lin, lin_other, soft, soft_other, weight, near_out, last_out, own_out):
    near_out[...] = dot(mixed_rows(index_ref, 1, lin, lin_other, soft, soft_other), weight[...]).astype(bf16)
    last_out[...] = dot(mixed_rows(index_ref, 2, lin, lin_other, soft, soft_other), weight[...])
    own_out[...] = dot(mixed_rows(index_ref, 3, lin, lin_other, soft, soft_other), weight[...])


def out_call(kernel, kinds, index, *operands):
    return pl.pallas_call(
        kernel,
        in_specs=[scalars()] + [whole()] * len(operands),
        out_shape=tuple(jax.ShapeDtypeStruct((ROWS, 1024), kind) for kind in kinds),
        compiler_params=params(14),
    )(index, *operands)


def shards(
    tokens, norm_gain, lin_query, lin_key, lin_value, lin_decay, decay_bias, decay_shift,
    soft_query, soft_key, soft_value, soft_lambda, lin_gain, soft_gain, lin_out, soft_out,
):
    x = lax.axis_index("fs")
    c = lax.axis_index("tp")
    z = lax.axis_index("sp_0")
    y = lax.axis_index("sp_1")
    head = x * 2 + c
    own = tokens[0]

    from_low = shift_fs(own, 1)
    from_high = shift_fs(own, 3)
    shifts = [jnp.pad(decay_shift.reshape(2, ROWS), ((0, EXTRA - 2), (0, 0)))]
    shifts += [shift_fs(shifts[0], 4 - d) for d in (1, 2, 3)]

    positions = (z * 4 + y) * ROWS + jnp.arange(ROWS, dtype=jnp.int32)
    inv_freq = jnp.power(f32(rope_base), -jnp.arange(64, dtype=f32) * (2.0 / KEY))
    angles = positions.astype(f32)[:, None] * inv_freq[None, :]
    cos = jnp.cos(angles)
    sin = jnp.sin(angles)
    cos_t = jnp.concatenate([cos, cos], axis=1)
    sin_t = jnp.concatenate([-sin, sin], axis=1)
    bias = lax.dynamic_slice_in_dim(decay_bias, head * KEY, KEY, 0).reshape(1, KEY)
    lam = lax.dynamic_slice_in_dim(soft_lambda, head, 1, 0)
    gain = norm_gain.reshape(1, -1)
    core = c.reshape(1)

    def run_front(chunk):
        other = swap(chunk)
        return front(core, chunk, other, gain, soft_key, soft_value, soft_query, cos_t, sin_t)

    def columns(matrix):
        half = matrix.shape[1] // 2
        mine = lax.dynamic_slice_in_dim(matrix, c * half, half, 1)
        return [mine, swap(lax.dynamic_slice_in_dim(matrix, (1 - c) * half, half, 1))]

    out_weight = jnp.concatenate(columns(lin_out) + columns(soft_out), axis=0)

    fronts = {0: run_front(own)}
    passed = jnp.where(c == 0, from_low, from_high)
    from_far = lax.ppermute(passed, ROW, core_ring(1))
    fronts[1] = run_front(from_high)
    fronts[3] = run_front(from_low)
    fronts[2] = run_front(from_far)
    kv, queries, normed = zip(*(fronts[d] for d in range(4)))
    kv, queries = jnp.stack(kv), jnp.stack(queries)
    local, carried, states = gla(normed, jnp.stack(shifts), (lin_value, lin_decay, lin_query, lin_key), bias)

    r = jnp.where(c == 0, z, y)
    q = jnp.where(c == 0, y, z)

    def piece(stacked, place, k):
        return lax.dynamic_index_in_dim(stacked, (place + k - x) & 3, 0, keepdims=False)

    own_kv = [piece(kv, r, 0)]
    for k in (1, 3, 2):
        own_kv.append(lax.ppermute(piece(kv, r, k), GRID, axis_perm(k, True)))
    own_kv = [own_kv[n] for n in (0, 1, 3, 2)]
    my_q = [lax.ppermute(piece(queries, r, k), GRID, query_perm(k)) for k in range(4)]
    y_parts = [piece(states, y, 0)]
    y_parts += [lax.ppermute(piece(states, y, k), "sp_1", ring(4, k)) for k in (1, 2, 3)]

    own_a = jnp.stack(own_kv[:2])
    own_b = jnp.stack(own_kv[2:])
    low_a = lax.ppermute(own_a, GRID, axis_perm(1, False))
    high_a = lax.ppermute(own_a, GRID, axis_perm(3, False))
    low_b = lax.ppermute(own_b, GRID, axis_perm(1, False))
    high_b = lax.ppermute(own_b, GRID, axis_perm(3, False))
    far_a = lax.ppermute(low_a, GRID, axis_perm(1, False))
    far_b = lax.ppermute(high_b, GRID, axis_perm(3, False))

    before, total = prefix(y.reshape(1), y_parts)
    z_parts = [total] + [lax.ppermute(total, "sp_0", ring(4, k)) for k in (1, 2, 3)]
    coming = combine(jnp.stack([z, y]), z_parts, before)
    coming = [coming[0]] + [lax.ppermute(coming[k], "sp_1", ring(4, k)) for k in (1, 2, 3)]
    k4 = jnp.arange(4, dtype=jnp.int32)
    lin_mix = lin_final((y - x - k4) & 3, coming, local, carried, lin_gain.reshape(1, -1))
    lin_other = swap(lin_mix)

    p = (r - k4) & 3
    source = jnp.where((p == 0) | (p == 3), q, 3 - q)
    ids = jnp.where(c == 0, 4 * p + source, 4 * source + p)
    k16 = jnp.arange(16, dtype=jnp.int32)
    away = jnp.where(k16 < 4, 0, jnp.where(k16 < 8, 1, jnp.where(k16 < 12, 3, 2)))
    block_p = (r - k16) & 3
    block_q = (q - away) & 3
    slot_ids = jnp.where(c == 0, 4 * block_p + block_q, 4 * block_q + block_p)
    sums = attend(
        True, ids, slot_ids[:12], lam, my_q, (own_a, own_b, low_a, low_b, high_a, high_b)
    )
    mix = attend(False, ids, slot_ids[12:], lam, my_q, (far_a, far_b), *sums, soft_gain.reshape(1, -1))

    soft_mix = jnp.stack([lax.ppermute(mix[k], GRID, query_perm(k, True)) for k in range(4)])
    lines = soft_mix[:, ROWS:].reshape(4, 2, 8, ROWS).astype(f32)
    mass_rows = lines[:, :, 0] + lines[:, :, 1] + lines[:, :, 2]
    log_mass = mass_rows[(k4 - r) & 3].transpose(1, 0, 2)[None]

    soft_other = swap(soft_mix)
    pieces = jnp.stack([jnp.int32(2), 3 - 2 * c, 1 + 2 * c, jnp.int32(0)])
    index = jnp.concatenate([pieces, (pieces + x - r) & 3, (pieces + x - q) & 3])
    rows = (lin_mix, lin_other, soft_mix, soft_other, out_weight)
    (far,) = out_call(send_kernel, (bf16,), index, *rows)
    passed = lax.ppermute(far, ROW, core_ring(1))
    near, last, mixed = out_call(keep_kernel, (bf16, f32, f32), index, *rows)
    near_in = lax.ppermute(near, ROW, core_ring(3))
    far_in = lax.ppermute((last + passed.astype(f32)).astype(bf16), ROW, core_ring(1))
    mixed = mixed + near_in.astype(f32) + far_in.astype(f32)
    return (mixed.astype(bf16)[None], log_mass)


def solution(mesh):
    split = Mesh(
        mesh.devices.reshape(4, 4, mesh.shape["fs"], mesh.shape["tp"]), ("sp_0", "sp_1", "fs", "tp")
    )
    heads = P(None, ("fs", "tp"))
    placed = (
        P("fs", SP, "tp"), P(), heads, heads, heads, heads, P(), P(None, "fs", SP),
        heads, heads, heads, P(), P(), P(), P(("fs", "tp"), None), P(("fs", "tp"), None),
    )

    return jax.shard_map(
        shards,
        mesh=split,
        in_specs=placed,
        out_specs=(P("fs", SP, "tp"), P(("fs", "tp"), None, None, SP)),
        check_vma=False,
    )
```

```python
from functools import partial
from types import SimpleNamespace

import jax
import jax.numpy as jnp
from jax import lax
from jax.experimental import pallas as pl
from jax.experimental.pallas import tpu as pltpu
from jax.sharding import Mesh
from jax.sharding import PartitionSpec as P


KEY = 128
VALUE = 256
SP = ("sp_0", "sp_1")
GRID = ("sp_0", "sp_1", "tp")
ROW = ("fs", "tp")
ROWS = 256
EXTRA = 16

norm_eps = 1e-06
decay_tau = 16.0
rope_base = 500000.0
LOG2E = 1.4426950408889634
LN2 = 0.6931471805599453

NT = (((1,), (1,)), ((), ()))
TN = (((0,), (0,)), ((), ()))
bf16 = jnp.bfloat16
f32 = jnp.float32


def dot(a, b, dims=(((1,), (0,)), ((), ()))):
    return lax.dot_general(a, b, dims, preferred_element_type=f32)


def ring(length, shift):
    return [(i, (i + shift) % length) for i in range(length)]


def axis_perm(shift, first):
    pairs = []
    for z in range(4):
        for y in range(4):
            for c in range(2):
                along_z = (c == 0) == first
                tz, ty = ((z + shift) % 4, y) if along_z else (z, (y + shift) % 4)
                pairs.append(((z * 4 + y) * 2 + c, (tz * 4 + ty) * 2 + c))
    return pairs


def query_perm(k, back=False):
    pairs = []
    for p in range(4):
        for o in range(4):
            for c in range(2):
                tp, to = (p + k) % 4, o if p in (0, 3) else 3 - o
                here, there = ((p, o), (tp, to)) if c == 0 else ((o, p), (to, tp))
                pairs.append(tuple((i * 4 + j) * 2 + c for i, j in ((there, here) if back else (here, there))))
    return pairs


def core_ring(shift):
    return [(x * 2 + c, ((x + (shift if c == 0 else 4 - shift)) % 4) * 2 + c) for x in range(4) for c in range(2)]


def shift_fs(array, shift):
    return lax.ppermute(array, "fs", ring(4, shift))


def swap(array):
    return lax.ppermute(array, "tp", ring(2, 1))


def scalars():
    return pl.BlockSpec(memory_space=pltpu.SMEM)


def whole():
    return pl.BlockSpec(memory_space=pltpu.VMEM)


def params(mib):
    return pltpu.CompilerParams(vmem_limit_bytes=mib * 1024 * 1024)


def front_kernel(core_ref, mine, other, gain, w_sk, w_sv, w_sq, cos_t, sin_t, kv_out, q_out, normed_out):
    x0 = mine[...].astype(f32)
    x1 = other[...].astype(f32)
    total = jnp.sum(x0 * x0, axis=1, keepdims=True) + jnp.sum(x1 * x1, axis=1, keepdims=True)
    inv = lax.rsqrt(total * (1.0 / 2048.0) + norm_eps)
    half = x0.shape[1]
    here = pl.multiple_of(core_ref[0] * half, half)
    there = pl.multiple_of((1 - core_ref[0]) * half, half)
    normed_out[:, pl.ds(here, half)] = (x0 * inv * gain[:, pl.ds(here, half)]).astype(bf16)
    normed_out[:, pl.ds(there, half)] = (x1 * inv * gain[:, pl.ds(there, half)]).astype(bf16)
    normed = normed_out[...]
    cos_v = cos_t[...]
    sin_v = sin_t[...]

    def rotate(values):
        return values * cos_v + pltpu.roll(values, 64, 1) * sin_v

    sk = dot(normed, w_sk[...])
    for m in range(2):
        kv_out[:, m * KEY : (m + 1) * KEY] = rotate(sk[:, m * KEY : (m + 1) * KEY]).astype(bf16)
    kv_out[:, 2 * KEY :] = dot(normed, w_sv[...]).T.astype(bf16)
    sq = dot(normed, w_sq[...])
    scale = (KEY ** (-0.5)) * LOG2E
    for m in range(2):
        q_out[m * KEY : (m + 1) * KEY, :] = (rotate(sq[:, m * KEY : (m + 1) * KEY]) * scale).T.astype(bf16)


def front(*operands):
    return pl.pallas_call(
        front_kernel,
        in_specs=[scalars()] + [whole()] * (len(operands) - 1),
        out_shape=tuple(jax.ShapeDtypeStruct((ROWS, cols), bf16) for cols in (4 * KEY, 2 * KEY, 2048)),
        compiler_params=params(14),
        cost_estimate=pl.CostEstimate(flops=1500000000, transcendentals=0, bytes_accessed=6000000),
    )(*operands)


def gla_kernel(
    n0, n1, n2, n3, shifts, w_lv, w_d, w_lq, w_lk, bias, local_out, carried_out, state_out, normed_ref, w_lqk
):
    for n, source in enumerate((n0, n1, n2, n3)):
        normed_ref[n] = source[...]
    w_lqk[:, :KEY] = w_lq[...]
    w_lqk[:, KEY:] = w_lk[...]

    def one(n, carry):
        gla_chunk(
            normed_ref[n], shifts[n], w_lv, w_d, w_lqk, bias, local_out.at[n], carried_out.at[n], state_out.at[n]
        )
        return carry

    lax.fori_loop(0, 4, one, 0)


def gla_chunk(normed, shift, w_lv, w_d, w_lqk, bias, local_out, carried_out, state_out):
    pick = lax.broadcasted_iota(jnp.int32, (EXTRA, KEY), 0)
    pick0 = jnp.where(pick == 0, 1.0, 0.0).astype(bf16)
    pick1 = jnp.where(pick == 1, 1.0, 0.0).astype(bf16)
    gate = dot(normed, w_d[...]) + bias[...] + dot(shift, pick0, TN)
    log_sig = jnp.minimum(gate, 0.0) - jnp.log1p(jnp.exp(-jnp.abs(gate)))
    log_decay = log_sig * (1.0 / decay_tau) + dot(shift, pick1, TN)
    v = dot(normed, w_lv[...]).astype(bf16)
    lqk = dot(normed, w_lqk[...])
    q = lqk[:, :KEY].astype(bf16).astype(f32)
    k = lqk[:, KEY:].astype(bf16).astype(f32)

    row = lax.broadcasted_iota(jnp.int32, (ROWS, KEY), 0)
    irow = lax.broadcasted_iota(jnp.int32, (KEY, KEY), 0)
    icol = lax.broadcasted_iota(jnp.int32, (KEY, KEY), 1)
    diff = irow ^ icol
    itself = jnp.sum(q * k, axis=1, keepdims=True)
    halves = [jnp.where(diff == 0, itself[n * KEY : (n + 1) * KEY], 0.0) for n in range(2)]
    inside = log_decay
    group = log_decay
    step = 1
    while step < ROWS:
        second = (row & step) != 0
        decay = jnp.exp(jnp.where(second, inside, group - inside))
        scaled = (jnp.where(second, q, k) * decay).astype(bf16)
        if 2 * step == ROWS:
            cross = dot(scaled[KEY:], scaled[:KEY], NT)
        else:
            keep = (diff < 2 * step) & ((irow & step) != 0) & ((icol & step) == 0)
            for n in range(2):
                part = scaled[n * KEY : (n + 1) * KEY]
                halves[n] = halves[n] + jnp.where(keep, dot(part, part, NT), 0.0)
        before = pltpu.roll(group, step, 0)
        after = pltpu.roll(group, ROWS - step, 0)
        inside = inside + jnp.where(second, before, 0.0)
        group = group + jnp.where(second, before, after)
        step *= 2
    local_out[:KEY] = dot(halves[0].astype(bf16), v[:KEY])
    local_out[KEY:] = dot(jnp.concatenate([cross, halves[1]], axis=1).astype(bf16), v)
    carried_out[...] = (q * jnp.exp(inside)).astype(bf16)
    kept = (k * jnp.exp(group - inside)).astype(bf16)
    state_out[:VALUE, :] = dot(v, kept, TN).astype(bf16)
    state_out[VALUE:, :] = jnp.exp(group[:EXTRA, :]).astype(bf16)


def gla(normed, shifts, weights, bias):
    return pl.pallas_call(
        gla_kernel,
        in_specs=[whole()] * 10,
        out_shape=(
            jax.ShapeDtypeStruct((4, ROWS, VALUE), f32),
            jax.ShapeDtypeStruct((4, ROWS, KEY), bf16),
            jax.ShapeDtypeStruct((4, VALUE + EXTRA, KEY), bf16),
        ),
        scratch_shapes=[pltpu.VMEM((4, ROWS, 2048), bf16), pltpu.VMEM((2048, 2 * KEY), bf16)],
        compiler_params=params(16),
        cost_estimate=pl.CostEstimate(flops=6000000000, transcendentals=0, bytes_accessed=9000000),
    )(*normed, shifts, *weights, bias)


def ordered(place, parts, j):
    k = (place - j) & 3
    value = parts[0]
    for n in range(1, 4):
        value = jnp.where(k == n, parts[n], value)
    return value


def prefix_kernel(place_ref, g0, g1, g2, g3, before_out, total_out):
    place = place_ref[0]
    parts = [g[...].astype(f32) for g in (g0, g1, g2, g3)]
    state = jnp.zeros((VALUE, KEY), f32)
    keep = jnp.ones((1, KEY), f32)
    for j in range(4):
        before_out[j, :VALUE, :] = state
        before_out[j, VALUE:, :] = jnp.broadcast_to(keep, (EXTRA, KEY))
        part = ordered(place, parts, j)
        own = part[VALUE : VALUE + 1, :]
        state = own * state + part[:VALUE, :]
        keep = own * keep
    total_out[:VALUE, :] = state.astype(bf16)
    total_out[VALUE:, :] = jnp.broadcast_to(keep, (EXTRA, KEY)).astype(bf16)


def prefix(place, parts):
    shape = (VALUE + EXTRA, KEY)
    return pl.pallas_call(
        prefix_kernel,
        in_specs=[scalars()] + [whole()] * 4,
        out_shape=(jax.ShapeDtypeStruct((4,) + shape, f32), jax.ShapeDtypeStruct(shape, bf16)),
        compiler_params=params(8),
    )(place, *parts)


def combine_kernel(place_ref, t0, t1, t2, t3, before, o0, o1, o2, o3):
    parts = [t[...].astype(f32) for t in (t0, t1, t2, t3)]
    state = jnp.zeros((VALUE, KEY), f32)
    chosen = state
    for j in range(4):
        chosen = jnp.where(place_ref[0] == j, state, chosen)
        part = ordered(place_ref[0], parts, j)
        state = part[VALUE : VALUE + 1, :] * state + part[:VALUE, :]
    for k, out in enumerate((o0, o1, o2, o3)):
        j = (place_ref[1] + k) & 3
        out[...] = (before[j, VALUE : VALUE + 1, :] * chosen + before[j, :VALUE, :]).astype(bf16)


def combine(places, totals, before):
    return pl.pallas_call(
        combine_kernel,
        in_specs=[scalars()] + [whole()] * 5,
        out_shape=tuple(jax.ShapeDtypeStruct((VALUE, KEY), bf16) for _ in range(4)),
        compiler_params=params(8),
    )(places, *totals, before)


def lin_kernel(index_ref, i0, i1, i2, i3, local, carried, gain, out):
    for n in range(4):
        which = index_ref[n]
        state_in = i0[...]
        for m, later in enumerate((i1, i2, i3)):
            state_in = jnp.where(which == m + 1, later[...], state_in)
        raw = local[n] + dot(carried[n], state_in, NT)
        mean = jnp.mean(raw * raw, axis=1, keepdims=True)
        out[n] = (raw * lax.rsqrt(mean + norm_eps) * gain[...]).astype(bf16)


def lin_final(index, states, local, carried, gain):
    return pl.pallas_call(
        lin_kernel,
        in_specs=[scalars()] + [whole()] * 7,
        out_shape=jax.ShapeDtypeStruct((4, ROWS, VALUE), bf16),
        compiler_params=params(12),
    )(index, *states, local, carried, gain)


def attend_kernel(near, ids_ref, slot_ids_ref, lam_ref, *refs):
    count_parts = 6 if near else 2
    q_refs, refs = refs[:4], refs[4:]
    parts, refs = refs[:count_parts], refs[count_parts:]
    if near:
        acc, top, total, items, q_all, kv, s_even, s_odd, p_even, p_odd, keep_even, keep_odd, sems = refs
    else:
        acc_in, top, total, gain, out0, out1, out2, out3, items, q_all, kv, s_even, s_odd, p_even, p_odd = refs[:15]
        keep_even, keep_odd, sems, acc, top_in, total_in, mass_ref, mix = refs[15:]
        top_in[...] = top[...]
        total_in[...] = total[...]
        top, total = top_in, total_in
        acc[...] = acc_in[...]
    copies = [
        pltpu.make_async_copy(source, kv.at[pl.ds(2 * n, 2)], sems.at[n]) for n, source in enumerate(parts)
    ]
    for copy in copies:
        copy.start()
    if near:
        acc[...] = jnp.zeros(acc.shape, f32)
        top[...] = jnp.full(top.shape, -jnp.inf, f32)
        total[...] = jnp.zeros(total.shape, f32)
    for n, source in enumerate(q_refs):
        q_all[n] = source[...]
    p_odd[...] = jnp.zeros(p_odd.shape, bf16)
    keep_odd[...] = jnp.ones(keep_odd.shape, f32)

    def collect(n, count):
        items[count] = n
        return count + jnp.where(slot_ids_ref[n >> 2] <= ids_ref[n & 3], 1, 0)

    count = lax.fori_loop(0, 8 * count_parts, collect, 0)
    visible = lax.broadcasted_iota(jnp.int32, (ROWS, ROWS), 0) <= lax.broadcasted_iota(jnp.int32, (ROWS, ROWS), 1)

    def item(i):
        n = items[i]
        return n >> 2, n & 3

    def arrive(slot, before):
        @pl.when((slot >> 1) != (before >> 1))
        def _():
            def wait(n, carry):
                pltpu.make_async_copy(parts[0], kv.at[pl.ds(2 * n, 2)], sems.at[n]).wait()
                return carry

            lax.fori_loop((before >> 1) + 1, (slot >> 1) + 1, wait, 0)

    def scores(after, slot, g, m):
        after[m] = dot(kv[slot, :, m * KEY : (m + 1) * KEY], q_all[g, m * KEY : (m + 1) * KEY, :])

    def mask(after, slot, g):
        @pl.when(slot_ids_ref[slot] == ids_ref[g])
        def _():
            for m in range(2):
                after[m] = jnp.where(visible, after[m], -jnp.inf)

    def weigh(now, p_now, keep_now, g, m):
        old = top[g, m][:1]
        peak = jnp.maximum(old, jnp.max(now[m], axis=0, keepdims=True))
        keep = jnp.exp2(old - peak)
        p = jnp.exp2(now[m] - peak)
        top[g, m] = jnp.broadcast_to(peak, (8, ROWS))
        total[g, m] = total[g, m] * keep + jnp.sum(p, axis=0, keepdims=True)
        keep_now[m] = jnp.broadcast_to(keep, (8, ROWS))
        p_now[m] = p.astype(bf16)

    def add(p_then, keep_then, slot, g, m):
        acc[g, m] = acc[g, m] * keep_then[m][:1] + dot(kv[slot, :, 2 * KEY :], p_then[m])

    def stage(i, now, after, p_now, p_then, keep_now, keep_then):
        slot_then, g_then = item(jnp.maximum(i - 1, 0))
        slot_now, g_now = item(i)
        slot_next, g_next = item(jnp.minimum(i + 1, count - 1))
        arrive(slot_next, slot_now)
        for m in range(2):
            scores(after, slot_next, g_next, m)
            weigh(now, p_now, keep_now, g_now, m)
            add(p_then, keep_then, slot_then, g_then, m)
        mask(after, slot_next, g_next)

    def run():
        first_slot, first_g = item(0)
        arrive(first_slot, -1)
        for m in range(2):
            scores(s_even, first_slot, first_g, m)
        mask(s_even, first_slot, first_g)

        def pair(n, carry):
            stage(2 * n, s_even, s_odd, p_even, p_odd, keep_even, keep_odd)

            @pl.when(2 * n + 1 < count)
            def _():
                stage(2 * n + 1, s_odd, s_even, p_odd, p_even, keep_odd, keep_even)

            return carry

        lax.fori_loop(0, (count + 1) >> 1, pair, 0)
        last_slot, last_g = item(count - 1)
        arrive(2 * count_parts - 1, last_slot)

        @pl.when((count & 1) == 1)
        def _():
            for m in range(2):
                add(p_even, keep_even, last_slot, last_g, m)

        @pl.when((count & 1) == 0)
        def _():
            for m in range(2):
                add(p_odd, keep_odd, last_slot, last_g, m)

    if near:
        pl.when(count > 0)(run)
        pl.when(count == 0)(lambda: arrive(2 * count_parts - 1, -1))
        return
    pl.when(count > 0)(run)
    pl.when(count == 0)(lambda: arrive(2 * count_parts - 1, -1))

    def finish(g, carry):
        sums = [total[g, m][:1] for m in range(2)]
        raw = acc[g, 0] * (1.0 / sums[0]) - acc[g, 1] * (lam_ref[0] / sums[1])
        mean = jnp.mean(raw * raw, axis=0, keepdims=True)
        mix[g, :ROWS] = ((raw * lax.rsqrt(mean + norm_eps)).T * gain[...]).astype(bf16)
        for m in range(2):
            left = jnp.broadcast_to(LN2 * top[g, m][:1] + jnp.log(sums[m]), (8, ROWS))
            lines = jnp.zeros((8, ROWS), f32)
            row = lax.broadcasted_iota(jnp.int32, (8, ROWS), 0)
            for n in range(3):
                part = left.astype(bf16).astype(f32)
                lines = jnp.where(row == n, part, lines)
                left = left - part
            mass_ref[m * 8 : (m + 1) * 8] = lines
        mix[g, ROWS:] = mass_ref[...].astype(bf16)
        return carry

    lax.fori_loop(0, 4, finish, 0)
    for n, out in enumerate((out0, out1, out2, out3)):
        out[...] = mix[n]


SUMS = ((4, 2, VALUE, ROWS), (4, 2, 8, ROWS), (4, 2, 8, ROWS))


def attend(near, ids, slot_ids, lam, queries, parts, *rest):
    scratch = [
        pltpu.SMEM((72,), jnp.int32),
        pltpu.VMEM((4, 2 * KEY, ROWS), bf16),
        pltpu.VMEM((2 * len(parts), ROWS, 4 * KEY), bf16),
        pltpu.VMEM((2, ROWS, ROWS), f32),
        pltpu.VMEM((2, ROWS, ROWS), f32),
        pltpu.VMEM((2, ROWS, ROWS), bf16),
        pltpu.VMEM((2, ROWS, ROWS), bf16),
        pltpu.VMEM((2, 8, ROWS), f32),
        pltpu.VMEM((2, 8, ROWS), f32),
        pltpu.SemaphoreType.DMA((len(parts),)),
    ]
    if near:
        out_shape = tuple(jax.ShapeDtypeStruct(shape, f32) for shape in SUMS)
    else:
        out_shape = tuple(jax.ShapeDtypeStruct((ROWS + EXTRA, VALUE), bf16) for _ in range(4))
        scratch += [pltpu.VMEM(shape, f32) for shape in SUMS]
        scratch += [pltpu.VMEM((EXTRA, ROWS), f32), pltpu.VMEM((4, ROWS + EXTRA, VALUE), bf16)]
    anywhere = pl.BlockSpec(memory_space=pl.ANY)
    return pl.pallas_call(
        partial(attend_kernel, near),
        in_specs=[scalars()] * 3 + [whole()] * 4 + [anywhere] * len(parts) + [whole()] * len(rest),
        out_shape=out_shape,
        scratch_shapes=scratch,
        compiler_params=params(18),
        cost_estimate=pl.CostEstimate(flops=4000000000, transcendentals=0, bytes_accessed=4000000),
    )(ids, slot_ids, lam, *queries, *parts, *rest)


def mixed_rows(index_ref, at, lin, lin_other, soft, soft_other):
    a = index_ref[at]
    b = index_ref[4 + at]
    e = index_ref[8 + at]
    return jnp.concatenate([lin[a], lin_other[a], soft[b, :ROWS], soft_other[e, :ROWS]], axis=1)


def send_kernel(index_ref, lin, lin_other, soft, soft_other, weight, far_out):
    far_out[...] = dot(mixed_rows(index_ref, 0, lin, lin_other, soft, soft_other), weight[...]).astype(bf16)


def keep_kernel(index_ref, lin, lin_other, soft, soft_other, weight, near_out, last_out, own_out):
    near_out[...] = dot(mixed_rows(index_ref, 1, lin, lin_other, soft, soft_other), weight[...]).astype(bf16)
    last_out[...] = dot(mixed_rows(index_ref, 2, lin, lin_other, soft, soft_other), weight[...])
    own_out[...] = dot(mixed_rows(index_ref, 3, lin, lin_other, soft, soft_other), weight[...])


def out_call(kernel, kinds, index, *operands):
    return pl.pallas_call(
        kernel,
        in_specs=[scalars()] + [whole()] * len(operands),
        out_shape=tuple(jax.ShapeDtypeStruct((ROWS, 1024), kind) for kind in kinds),
        compiler_params=params(14),
    )(index, *operands)


def shards(
    tokens, norm_gain, lin_query, lin_key, lin_value, lin_decay, decay_bias, decay_shift,
    soft_query, soft_key, soft_value, soft_lambda, lin_gain, soft_gain, lin_out, soft_out,
):
    x = lax.axis_index("fs")
    c = lax.axis_index("tp")
    z = lax.axis_index("sp_0")
    y = lax.axis_index("sp_1")
    head = x * 2 + c
    k4 = jnp.arange(4, dtype=jnp.int32)
    k16 = jnp.arange(16, dtype=jnp.int32)
    r = jnp.where(c == 0, z, y)
    q = jnp.where(c == 0, y, z)
    p = (r - k4) & 3
    source = jnp.where((p == 0) | (p == 3), q, 3 - q)
    ids = jnp.where(c == 0, 4 * p + source, 4 * source + p)
    away = jnp.where(k16 < 4, 0, jnp.where(k16 < 8, 1, jnp.where(k16 < 12, 3, 2)))
    block_p = (r - k16) & 3
    block_q = (q - away) & 3
    slot_ids = jnp.where(c == 0, 4 * block_p + block_q, 4 * block_q + block_p)
    pieces = jnp.stack([jnp.int32(2), 3 - 2 * c, 1 + 2 * c, jnp.int32(0)])
    index = jnp.concatenate([pieces, (pieces + x - r) & 3, (pieces + x - q) & 3])
    place = dict(
        core=c.reshape(1), first=c == 0, ids=ids, near_ids=slot_ids[:12], far_ids=slot_ids[12:], index=index,
        r_pieces=[(r + k - x) & 3 for k in range(4)], y_pieces=[(y + k - x) & 3 for k in range(4)],
        y=y.reshape(1), zy=jnp.stack([z, y]), lin=(y - x - k4) & 3, order=(k4 - r) & 3,
        own_columns=c * 1024, other_columns=(1 - c) * 1024,
        head=head, bias_at=head * KEY,
    )
    positions = (z * 4 + y) * ROWS + jnp.arange(ROWS, dtype=jnp.int32)
    tokens, place = lax.optimization_barrier((tokens, place))
    place = SimpleNamespace(**place)
    own = tokens[0]

    from_low = shift_fs(own, 1)
    from_high = shift_fs(own, 3)
    shifts = [jnp.pad(decay_shift.reshape(2, ROWS), ((0, EXTRA - 2), (0, 0)))]
    shifts += [shift_fs(shifts[0], 4 - d) for d in (1, 2, 3)]

    inv_freq = jnp.power(f32(rope_base), -jnp.arange(64, dtype=f32) * (2.0 / KEY))
    angles = positions.astype(f32)[:, None] * inv_freq[None, :]
    cos = jnp.cos(angles)
    sin = jnp.sin(angles)
    cos_t = jnp.concatenate([cos, cos], axis=1)
    sin_t = jnp.concatenate([-sin, sin], axis=1)
    gain = norm_gain.reshape(1, -1)
    core = place.core
    bias = lax.dynamic_slice(decay_bias, (place.bias_at,), (KEY,), allow_negative_indices=False).reshape(1, KEY)
    lam = lax.dynamic_slice(soft_lambda, (place.head,), (1,), allow_negative_indices=False)

    def run_front(chunk):
        other = swap(chunk)
        return front(core, chunk, other, gain, soft_key, soft_value, soft_query, cos_t, sin_t)

    def columns_at(matrix, at, half):
        return lax.dynamic_slice(matrix, (0, at), (matrix.shape[0], half), allow_negative_indices=False)

    def columns(matrix):
        half = matrix.shape[1] // 2
        mine = columns_at(matrix, place.own_columns, half)
        return [mine, swap(columns_at(matrix, place.other_columns, half))]

    out_weight = jnp.concatenate(columns(lin_out) + columns(soft_out), axis=0)

    fronts = {0: run_front(own)}
    passed = jnp.where(place.first, from_low, from_high)
    from_far = lax.ppermute(passed, ROW, core_ring(1))
    fronts[1] = run_front(from_high)
    fronts[3] = run_front(from_low)
    fronts[2] = run_front(from_far)
    kv, queries, normed = zip(*(fronts[d] for d in range(4)))
    kv, queries = jnp.stack(kv), jnp.stack(queries)
    local, carried, states = gla(normed, jnp.stack(shifts), (lin_value, lin_decay, lin_query, lin_key), bias)

    def piece(stacked, at):
        sizes = (1,) + stacked.shape[1:]
        return lax.dynamic_slice(stacked, (at, 0, 0), sizes, allow_negative_indices=False)[0]

    by_r, by_y = place.r_pieces, place.y_pieces
    own_kv = [piece(kv, by_r[0])]
    for k in (1, 3, 2):
        own_kv.append(lax.ppermute(piece(kv, by_r[k]), GRID, axis_perm(k, True)))
    own_kv = [own_kv[n] for n in (0, 1, 3, 2)]
    my_q = [lax.ppermute(piece(queries, by_r[k]), GRID, query_perm(k)) for k in range(4)]
    y_parts = [piece(states, by_y[0])]
    y_parts += [lax.ppermute(piece(states, by_y[k]), "sp_1", ring(4, k)) for k in (1, 2, 3)]

    own_a = jnp.stack(own_kv[:2])
    own_b = jnp.stack(own_kv[2:])
    low_a = lax.ppermute(own_a, GRID, axis_perm(1, False))
    high_a = lax.ppermute(own_a, GRID, axis_perm(3, False))
    low_b = lax.ppermute(own_b, GRID, axis_perm(1, False))
    high_b = lax.ppermute(own_b, GRID, axis_perm(3, False))
    far_a = lax.ppermute(low_a, GRID, axis_perm(1, False))
    far_b = lax.ppermute(high_b, GRID, axis_perm(3, False))

    before, total = prefix(place.y, y_parts)
    z_parts = [total] + [lax.ppermute(total, "sp_0", ring(4, k)) for k in (1, 2, 3)]
    coming = combine(place.zy, z_parts, before)
    coming = [coming[0]] + [lax.ppermute(coming[k], "sp_1", ring(4, k)) for k in (1, 2, 3)]
    lin_mix = lin_final(place.lin, coming, local, carried, lin_gain.reshape(1, -1))
    lin_other = swap(lin_mix)

    sums = attend(
        True, place.ids, place.near_ids, lam, my_q, (own_a, own_b, low_a, low_b, high_a, high_b)
    )
    mix = attend(
        False, place.ids, place.far_ids, lam, my_q, (far_a, far_b), *sums,
        soft_gain.reshape(1, -1),
    )

    soft_mix = jnp.stack([lax.ppermute(mix[k], GRID, query_perm(k, True)) for k in range(4)])
    lines = soft_mix[:, ROWS:].reshape(4, 2, 8, ROWS).astype(f32)
    mass_rows = lines[:, :, 0] + lines[:, :, 1] + lines[:, :, 2]
    log_mass = mass_rows[place.order].transpose(1, 0, 2)[None]

    soft_other = swap(soft_mix)
    index = place.index
    rows = (lin_mix, lin_other, soft_mix, soft_other, out_weight)
    (far,) = out_call(send_kernel, (bf16,), index, *rows)
    passed = lax.ppermute(far, ROW, core_ring(1))
    near, last, mixed = out_call(keep_kernel, (bf16, f32, f32), index, *rows)
    near_in = lax.ppermute(near, ROW, core_ring(3))
    far_in = lax.ppermute((last + passed.astype(f32)).astype(bf16), ROW, core_ring(1))
    mixed = mixed + near_in.astype(f32) + far_in.astype(f32)
    return (mixed.astype(bf16)[None], log_mass)


def solution(mesh):
    split = Mesh(
        mesh.devices.reshape(4, 4, mesh.shape["fs"], mesh.shape["tp"]), ("sp_0", "sp_1", "fs", "tp")
    )
    heads = P(None, ("fs", "tp"))
    placed = (
        P("fs", SP, "tp"), P(), heads, heads, heads, heads, P(), P(None, "fs", SP),
        heads, heads, heads, P(), P(), P(), P(("fs", "tp"), None), P(("fs", "tp"), None),
    )

    return jax.shard_map(
        shards,
        mesh=split,
        in_specs=placed,
        out_specs=(P("fs", SP, "tp"), P(("fs", "tp"), None, None, SP)),
        check_vma=False,
    )
```
